32 devices in a mesh: rep: 2 (over x), fs: 4 (over z), tp: 4 (over y, core).
Axes of the slice: x: 2, y: 2, z: 4, core: 2. Of those that a mesh axis runs over, the one named last changes fastest.
Arguments:
- residual: bfloat16 [8, 768, 4, 512], P(('rep', 'fs'), None, None, 'tp'), may hold values from -6 to 6
- mixer_gain: float32 [4, 512], P(None, 'tp'), may hold values from 0.1 to 1.9
- pool_weight: float32 [4, 512, 512], P(None, 'fs', 'tp'), may hold values from -0.25 to 0.25
- pool_scale: float32 [4, 512], P(None, 'tp'), may hold values from 0.5 to 2
- channel_gain: float32 [4, 512], P(None, 'tp'), may hold values from 0.1 to 1.9
- gate_weight: float32 [2048, 6144], P('fs', 'tp'), may hold values from -0.125 to 0.125
- up_weight: float32 [2048, 6144], P('fs', 'tp'), may hold values from -0.125 to 0.125
- gate_scale: float32 [4, 1536], P('fs', 'tp'), may hold values from 0.5 to 2
- up_scale: float32 [4, 1536], P('fs', 'tp'), may hold values from 0.5 to 2
- gate_taps: float32 [3, 6144], P(None, 'tp'), may hold values from -3.5 to 3.5
- up_taps: float32 [3, 6144], P(None, 'tp'), may hold values from -3.5 to 3.5
- down_weight: float32 [6144, 2048], P('tp', 'fs'), may hold values from -0.078125 to 0.078125
- down_scale: float32 [4, 512], P(None, 'tp'), may hold values from 0.5 to 2
Outputs:
- layer_out: bfloat16 [8, 768, 4, 512], P(('rep', 'fs'), None, None, 'tp')
The draws below stay inside these ranges and needn't reach their ends.
All inputs are finite; a program needn't handle non-finite values.
Results may differ from the reference program's by a relative error of at most 0.018.
Values may be sent and summed in bfloat16 or wider, within the bound.
No kernel may reach another device: no remote copies, remote signals or barrier semaphores. Data moves between devices by JAX's collectives and lax.ppermute only.
A program may use at most 128 MiB of HBM per device.

```python
import math
import jax
import jax.numpy as jnp
from jax import lax

D = 2048
G = 4
C = 512
FF = 6144
SEQ_LEN = 768
SEQS = 8
N_FS = 4
N_TP = 4


def level_of(own_key, shape, shards, least, largest):
    level = 1.0
    for position, parts in shards:
        draws = jax.random.uniform(jax.random.fold_in(jax.random.fold_in(own_key, 6), position), (parts,), jnp.float32, least / len(shards), largest / len(shards))
        level = level * jnp.repeat(jnp.exp(draws), shape[position] // parts).reshape((-1,) + (1,) * (len(shape) - 1 - position))
    return level


def gaussian(rng, shape, scale, reach, shards=(), kind=jnp.bfloat16):
    level = level_of(rng, shape, shards, -0.22, 0.18) if shards else 1.0
    values = jax.random.normal(rng, shape, jnp.float32) * scale * level
    return jnp.minimum(jnp.maximum(values, -reach), reach).astype(kind)


def setup_inputs(seed: int = 0) -> dict:
    key_list = jax.random.split(jax.random.key(seed), 14)
    residual = gaussian(key_list[0], (SEQS, SEQ_LEN, G, C), 1.0, 6.0, ((0, 8), (3, 4)))
    mixer_gain = jnp.clip(1.0 + 0.18 * jax.random.normal(key_list[1], (G, C), jnp.float32), 0.1, 1.9)
    pool_weight = gaussian(key_list[2], (G, C, C), C ** -0.5, 0.25, ((1, 4), (2, 4)), jnp.float32)
    pool_scale = jnp.clip(jnp.exp(math.log(2.0) - 1.3862944 * jax.random.uniform(key_list[3], (G, C), jnp.float32) ** level_of(key_list[3], (G, C), ((1, 4),), -0.2, 0.2)), 0.5, 2.0)
    channel_gain = jnp.clip(1.0 + 0.18 * jax.random.normal(key_list[4], (G, C), jnp.float32), 0.1, 1.9)
    gate_weight = gaussian(key_list[5], (D, FF), D ** -0.5, 0.125, ((0, 4), (1, 4)), jnp.float32)
    up_weight = gaussian(key_list[6], (D, FF), D ** -0.5, 0.125, ((0, 4), (1, 4)), jnp.float32)
    gate_scale = jnp.clip(jnp.exp(math.log(2.0) - 1.3862944 * jax.random.uniform(key_list[7], (N_FS, FF // N_FS), jnp.float32) ** level_of(key_list[7], (N_FS, FF // N_FS), ((0, 4), (1, 4)), -0.2, 0.2)), 0.5, 2.0)
    up_scale = jnp.clip(jnp.exp(math.log(2.0) - 1.3862944 * jax.random.uniform(key_list[8], (N_FS, FF // N_FS), jnp.float32) ** level_of(key_list[8], (N_FS, FF // N_FS), ((0, 4), (1, 4)), -0.2, 0.2)), 0.5, 2.0)
    gate_taps = gaussian(key_list[9], (3, FF), 3 ** -0.5, 3.5, ((1, 4),), jnp.float32)
    up_taps = gaussian(key_list[10], (3, FF), 3 ** -0.5, 3.5, ((1, 4),), jnp.float32)
    down_weight = gaussian(key_list[11], (FF, D), FF ** -0.5, 0.078125, ((0, 4), (1, 4)), jnp.float32)
    down_scale = jnp.clip(jnp.exp(math.log(2.0) - 1.3862944 * jax.random.uniform(key_list[12], (G, C), jnp.float32) ** level_of(key_list[12], (G, C), ((1, 4),), -0.2, 0.2)), 0.5, 2.0)
    return dict(residual=residual, mixer_gain=mixer_gain, pool_weight=pool_weight, pool_scale=pool_scale, channel_gain=channel_gain, gate_weight=gate_weight, up_weight=up_weight, gate_scale=gate_scale, up_scale=up_scale, gate_taps=gate_taps, up_taps=up_taps, down_weight=down_weight, down_scale=down_scale)


WINDOWS = (2, 4, 8, 16)
EPSILON = 1e-05

def shifted(values, steps):
    padding = jnp.zeros((steps,) + values.shape[1:], values.dtype)
    return jnp.concatenate([padding, values[:-steps]], axis=0)

def pooled_groups(normed):
    values = normed.astype(jnp.float32)
    totals = values
    reach_now = 1
    columns = []
    positions = jnp.arange(1, values.shape[0] + 1).astype(jnp.float32)
    for group_idx in range(len(WINDOWS)):
        while reach_now < WINDOWS[group_idx]:
            totals = totals + shifted(totals, reach_now)
            reach_now = reach_now * 2
        divisor = jnp.minimum(positions, float(WINDOWS[group_idx]))
        columns.append(totals[:, group_idx] / divisor[:, None] - values[:, group_idx])
    return jnp.stack(columns, axis=1).astype(jnp.bfloat16)

def normalized(residual, gain):
    values = residual.astype(jnp.float32)
    mean_square = lax.optimization_barrier(jnp.mean(values * values, axis=(1, 2), keepdims=True))
    return (values * lax.rsqrt(mean_square + EPSILON) * gain).astype(jnp.bfloat16)

def causal_taps(stored, taps):
    values = stored.astype(jnp.float32)
    return taps[2] * values + taps[1] * shifted(values, 1) + taps[0] * shifted(values, 2)

def shard_order(scale):
    return jnp.transpose(scale.reshape(N_FS, N_TP, -1), (1, 0, 2)).reshape(-1)

def one_sequence(residual, mixer_gain, pool_half, pool_scale, channel_gain, gate_half, up_half, gate_columns, up_columns, gate_taps, up_taps, down_half, down_scale):
    normed = normalized(residual, mixer_gain)
    pooled = pooled_groups(normed)
    mixed = jnp.einsum('lgc,gce->lge', pooled.astype(jnp.float32), pool_half.astype(jnp.float32))
    middle = (mixed * pool_scale + residual.astype(jnp.float32)).astype(jnp.bfloat16)
    length = middle.shape[0]
    inputs = normalized(middle, channel_gain).reshape(length, -1)
    gate_pre = (jnp.dot(inputs, gate_half, preferred_element_type=jnp.float32) * gate_columns).astype(jnp.bfloat16)
    up_pre = (jnp.dot(inputs, up_half, preferred_element_type=jnp.float32) * up_columns).astype(jnp.bfloat16)
    hidden = (jax.nn.silu(causal_taps(gate_pre, gate_taps)) * causal_taps(up_pre, up_taps)).astype(jnp.bfloat16)
    block_rows = hidden.shape[1] // N_TP
    summed = jnp.zeros((length, down_half.shape[1]), jnp.float32)
    for shard_idx in range(N_TP):
        lower = shard_idx * block_rows
        partial_sum = jnp.dot(hidden[:, lower:lower + block_rows], down_half[lower:lower + block_rows], preferred_element_type=jnp.float32).astype(jnp.bfloat16)
        summed = summed + lax.optimization_barrier(partial_sum).astype(jnp.float32)
    summed = summed.reshape(middle.shape)
    return (summed * down_scale + middle.astype(jnp.float32)).astype(jnp.bfloat16)

def reference(residual, mixer_gain, pool_weight, pool_scale, channel_gain, gate_weight, up_weight, gate_scale, up_scale, gate_taps, up_taps, down_weight, down_scale):
    pool_half = pool_weight.astype(jnp.bfloat16)
    gate_half = gate_weight.astype(jnp.bfloat16)
    up_half = up_weight.astype(jnp.bfloat16)
    down_half = down_weight.astype(jnp.bfloat16)
    gate_columns = shard_order(gate_scale)
    up_columns = shard_order(up_scale)

    def per_sequence(sequence):
        return one_sequence(sequence, mixer_gain, pool_half, pool_scale, channel_gain, gate_half, up_half, gate_columns, up_columns, gate_taps, up_taps, down_half, down_scale)
    return lax.map(per_sequence, residual)
```

```python
import jax
import jax.numpy as jnp
from jax import lax
from jax.sharding import PartitionSpec as P

WINDOWS = (2, 4, 8, 16)
EPSILON = 1e-05


def shifted(values, steps):
    padding = jnp.zeros((steps,) + values.shape[1:], values.dtype)
    return jnp.concatenate([padding, values[:-steps]], axis=0)


def pooled_groups(normed):
    values = normed.astype(jnp.float32)
    totals = values
    reach_now = 1
    columns = []
    positions = jnp.arange(1, values.shape[0] + 1).astype(jnp.float32)
    for group_idx in range(len(WINDOWS)):
        while reach_now < WINDOWS[group_idx]:
            totals = totals + shifted(totals, reach_now)
            reach_now = reach_now * 2
        divisor = jnp.minimum(positions, float(WINDOWS[group_idx]))
        columns.append(totals[:, group_idx] / divisor[:, None] - values[:, group_idx])
    return jnp.stack(columns, axis=1).astype(jnp.bfloat16)


def local_square(values):
    return jnp.sum(values * values, axis=(1, 2), keepdims=True)


def scaled(values, total, width_all, gain):
    return (values * lax.rsqrt(total / width_all + EPSILON) * gain).astype(jnp.bfloat16)


def causal_taps(stored, taps):
    values = stored.astype(jnp.float32)
    return taps[2] * values + taps[1] * shifted(values, 1) + taps[0] * shifted(values, 2)


def plain_shards(
    residual,
    mixer_gain,
    pool_weight,
    pool_scale,
    channel_gain,
    gate_weight,
    up_weight,
    gate_scale,
    up_scale,
    gate_taps,
    up_taps,
    down_weight,
    down_scale,
):
    sequence = residual[0]
    length = sequence.shape[0]
    groups = sequence.shape[1]
    local_width = sequence.shape[2]
    width_all = groups * local_width * lax.axis_size("tp")
    pool_rows = lax.all_gather(pool_weight.astype(jnp.bfloat16), "fs", axis=1, tiled=True)
    values = sequence.astype(jnp.float32)
    total = lax.psum(local_square(values), "tp")
    pooled = pooled_groups(scaled(values, total, width_all, mixer_gain))
    mixed = jnp.einsum(
        "lgc,gce->lge",
        lax.all_gather(pooled, "tp", axis=2, tiled=True),
        pool_rows,
        preferred_element_type=jnp.float32,
    )
    middle = (mixed * pool_scale + values).astype(jnp.bfloat16)
    middle_values = middle.astype(jnp.float32)
    middle_total = lax.psum(local_square(middle_values), "tp")
    inputs_local = scaled(middle_values, middle_total, width_all, channel_gain)
    inputs = lax.all_gather(inputs_local, "tp", axis=2, tiled=True).reshape(length, -1)
    scale_pair = (
        lax.all_gather(gate_scale, "fs", axis=0, tiled=True),
        lax.all_gather(up_scale, "fs", axis=0, tiled=True),
    )
    gate_columns = scale_pair[0].reshape(-1)
    up_columns = scale_pair[1].reshape(-1)
    gate_half = gate_weight.astype(jnp.bfloat16)
    up_half = up_weight.astype(jnp.bfloat16)
    gate_full, up_full = (
        lax.all_gather(gate_half, "fs", axis=0, tiled=True),
        lax.all_gather(up_half, "fs", axis=0, tiled=True),
    )
    gate_acc = jnp.dot(inputs, gate_full, preferred_element_type=jnp.float32)
    up_acc = jnp.dot(inputs, up_full, preferred_element_type=jnp.float32)
    gate_pre = (gate_acc * gate_columns).astype(jnp.bfloat16)
    up_pre = (up_acc * up_columns).astype(jnp.bfloat16)
    hidden = (jax.nn.silu(causal_taps(gate_pre, gate_taps)) * causal_taps(up_pre, up_taps)).astype(
        jnp.bfloat16
    )
    down_full = lax.all_gather(down_weight.astype(jnp.bfloat16), "fs", axis=1, tiled=True)
    down_grouped = down_full.reshape(down_full.shape[0], groups, -1)
    summed_rows = lax.psum_scatter(
        jnp.einsum("lf,fgc->clg", hidden, down_grouped, preferred_element_type=jnp.float32).astype(
            jnp.bfloat16
        ),
        "tp",
        scatter_dimension=0,
        tiled=True,
    ).astype(jnp.float32)
    summed = jnp.transpose(summed_rows, (1, 2, 0))
    layer_out = (summed * down_scale + middle_values).astype(jnp.bfloat16)
    return layer_out[None]


def exchanged(values, axis, bit):
    size = lax.axis_size(axis)
    return lax.ppermute(values, axis, [(place, place ^ bit) for place in range(size)])


def gathered_slots(values, axis):
    slots = [values]
    for slot_idx in range(1, lax.axis_size(axis)):
        low_bit = slot_idx & -slot_idx
        slots.append(exchanged(slots[slot_idx ^ low_bit], axis, low_bit))
    return slots


def index_ordered(stacked, axis):
    size = stacked.shape[0]
    own = lax.axis_index(axis)
    bit = 1
    while bit < size:
        pairs = stacked.reshape((size // (2 * bit), 2, bit) + stacked.shape[1:])
        swapped = jnp.flip(pairs, axis=1).reshape(stacked.shape)
        stacked = jnp.where((own & bit) != 0, swapped, stacked)
        bit *= 2
    return stacked


def half_of(values, axis, dimension):
    width = values.shape[dimension] // lax.axis_size(axis)
    return lax.dynamic_slice_in_dim(values, lax.axis_index(axis) * width, width, dimension)


def stage_one(rows, mixer_gain, pool_full, pool_scale, channel_gain):
    values = rows.astype(jnp.float32)
    width_all = values.shape[1] * values.shape[2]
    pooled = pooled_groups(scaled(values, local_square(values), width_all, mixer_gain))
    mixed = jnp.einsum("lgc,gce->lge", pooled, pool_full, preferred_element_type=jnp.float32)
    middle = (mixed * pool_scale + values).astype(jnp.bfloat16)
    middle_values = middle.astype(jnp.float32)
    inputs = scaled(middle_values, local_square(middle_values), width_all, channel_gain)
    return middle, inputs.reshape(inputs.shape[0], -1)


def shards(
    residual,
    mixer_gain,
    pool_weight,
    pool_scale,
    channel_gain,
    gate_weight,
    up_weight,
    gate_scale,
    up_scale,
    gate_taps,
    up_taps,
    down_weight,
    down_scale,
):
    sequence = residual[0]
    length, groups, local_width = sequence.shape
    reps = lax.axis_size("rep")
    fs_size = lax.axis_size("fs")
    tp_size = lax.axis_size("tp")
    channels = local_width * tp_size
    pool_half = pool_weight.astype(jnp.bfloat16)
    pool_slots = jnp.stack(gathered_slots(pool_half, "fs"))
    gate_half = half_of(gate_weight, "rep", 1).astype(jnp.bfloat16)
    up_half = half_of(up_weight, "rep", 1).astype(jnp.bfloat16)
    down_half = half_of(down_weight, "rep", 0).astype(jnp.bfloat16)
    gate_slots = gathered_slots(gate_half, "fs")
    up_slots = gathered_slots(up_half, "fs")
    down_half, _ = lax.optimization_barrier((down_half, gate_slots[-1]))
    down_slots = gathered_slots(down_half, "fs")
    vectors = jnp.stack([mixer_gain, pool_scale, channel_gain])
    vectors = index_ordered(jnp.stack(gathered_slots(vectors, "tp")), "tp")
    vectors = jnp.moveaxis(vectors, 0, 2).reshape(3, groups, channels)
    scales = jnp.concatenate([gate_scale, up_scale])
    scales = index_ordered(jnp.stack(gathered_slots(scales, "fs")), "fs")
    scales = half_of(jnp.moveaxis(scales, 0, 1).reshape(2, -1), "rep", 1)
    flat = sequence.reshape(length, groups * local_width)
    row_slots = jnp.stack(
        [jnp.stack(gathered_slots(slot, "tp")) for slot in gathered_slots(flat, "rep")], axis=1
    )
    rows = index_ordered(row_slots, "tp").reshape(tp_size, reps, length, groups, local_width)
    rows = jnp.transpose(rows, (1, 2, 3, 0, 4)).reshape(reps, length, groups, channels)
    pool_full = index_ordered(jnp.stack(gathered_slots(pool_slots, "tp")), "tp")
    pool_full = jnp.moveaxis(index_ordered(jnp.moveaxis(pool_full, 1, 0), "fs"), 0, 1)
    pool_full = jnp.transpose(pool_full, (2, 1, 3, 0, 4)).reshape(groups, channels, channels)
    middle, inputs = jax.vmap(
        lambda part: stage_one(part, vectors[0], pool_full, vectors[1], vectors[2])
    )(rows)
    own_middle = lax.dynamic_slice_in_dim(
        middle[0], lax.axis_index("tp") * local_width, local_width, 2
    ).astype(jnp.float32)
    gate_full = index_ordered(jnp.stack(gate_slots), "fs").reshape(groups * channels, -1)
    up_full = index_ordered(jnp.stack(up_slots), "fs").reshape(groups * channels, -1)
    gate_acc = jnp.einsum("rlk,kh->rlh", inputs, gate_full, preferred_element_type=jnp.float32)
    up_acc = jnp.einsum("rlk,kh->rlh", inputs, up_full, preferred_element_type=jnp.float32)
    gate_pre = (gate_acc * scales[0]).astype(jnp.bfloat16)
    up_pre = (up_acc * scales[1]).astype(jnp.bfloat16)
    gate_half_taps = half_of(gate_taps, "rep", 1)
    up_half_taps = half_of(up_taps, "rep", 1)
    conv_gate = jax.vmap(lambda part: causal_taps(part, gate_half_taps))(gate_pre)
    conv_up = jax.vmap(lambda part: causal_taps(part, up_half_taps))(up_pre)
    hidden = (jax.nn.silu(conv_gate) * conv_up).astype(jnp.bfloat16)
    finished = []
    for down_slot in down_slots:
        partial_sums = jnp.einsum(
            "rlh,hc->rlc", hidden, down_slot, preferred_element_type=jnp.float32
        ).astype(jnp.bfloat16)
        blocks = partial_sums.reshape(reps, length, -1, tp_size, local_width)
        blocks = index_ordered(jnp.transpose(blocks, (3, 0, 1, 2, 4)), "tp")
        bit = 1
        while bit < tp_size:
            pairs = blocks.reshape((-1, 2) + blocks.shape[1:])
            blocks = (
                pairs[:, 0].astype(jnp.float32)
                + exchanged(pairs[:, 1], "tp", bit).astype(jnp.float32)
            ).astype(jnp.bfloat16)
            bit *= 2
        blocks = blocks[0]
        bit = 1
        while bit < reps:
            pairs = blocks.reshape((-1, 2) + blocks.shape[1:])
            blocks = pairs[:, 0].astype(jnp.float32) + exchanged(
                pairs[:, 1], "rep", bit
            ).astype(jnp.float32)
            bit *= 2
        finished.append(blocks[0])
    summed = index_ordered(jnp.stack(finished), "fs")
    summed = jnp.moveaxis(summed, 0, 1).reshape(length, groups, local_width)
    layer_out = (summed.astype(jnp.float32) * down_scale + own_middle).astype(jnp.bfloat16)
    return layer_out[None]


def is_power_of_two(size):
    return size & (size - 1) == 0


def solution(mesh):
    placed = (
        P(("rep", "fs"), None, None, "tp"),
        P(None, "tp"),
        P(None, "fs", "tp"),
        P(None, "tp"),
        P(None, "tp"),
        P("fs", "tp"),
        P("fs", "tp"),
        P("fs", "tp"),
        P("fs", "tp"),
        P(None, "tp"),
        P(None, "tp"),
        P("tp", "fs"),
        P(None, "tp"),
    )
    sizes = dict(mesh.shape)
    split = all(is_power_of_two(size) for size in sizes.values())

    def chosen(*parts):
        groups, channels = parts[1].shape[0], parts[2].shape[1] * sizes["fs"]
        whole_groups = parts[11].shape[1] % channels == 0
        return (shards if split and whole_groups else plain_shards)(*parts)

    return jax.shard_map(
        chosen,
        mesh=mesh,
        in_specs=placed,
        out_specs=P(("rep", "fs"), None, None, "tp"),
        check_vma=False,
    )
```
